32 devices in a mesh: rep: 2 (over x), fs: 8 (over z, y), tp: 2 (over core).
Axes of the slice: x: 2, y: 2, z: 4, core: 2. Of those that a mesh axis runs over, the one named last changes fastest.
Arguments:
- inputs: bfloat16 [6144, 2048], P(('rep', 'fs')), may hold values from -6 to 6
- w_up: bfloat16 [2048, 4096], P('fs', 'tp'), may hold values from -0.125 to 0.125
- w_down: bfloat16 [4096, 2048], P('tp', 'fs'), may hold values from -0.09375 to 0.09375
- cotangent: bfloat16 [6144, 2048], P(('rep', 'fs')), may hold values from -6 to 6
Outputs:
- d_inputs: bfloat16 [6144, 2048], P(('rep', 'fs'))
- d_w_up: float32 [2048, 4096], P('fs', 'tp')
The draws below stay inside these ranges and needn't reach their ends.
All inputs are finite; a program needn't handle non-finite values.
Results may differ from the reference program's by a relative error of at most 0.014.
Values may be sent and summed in bfloat16 or wider, within the bound.
A program may use at most 128 MiB of HBM per device.

```python
import jax
import jax.numpy as jnp

D = 2048
FF = 4096
TOKENS = 6144
N_TP = 2


def strengthened(result, own_key, source, target, shards_of, factor):
    def block_of(axis_at):
        return (jnp.arange(result.shape[axis_at]) // (result.shape[axis_at] // shards_of)).reshape((-1,) + (1,) * (result.ndim - 1 - axis_at))

    near = jax.random.permutation(own_key, shards_of)[block_of(target)]
    other_side = (block_of(target) + shards_of // 2) % shards_of
    return jnp.where((block_of(source) == near) | (block_of(source) == other_side), factor * result, result)


def block_levels(key, extent, pieces, low, top_value):
    def one(dim, blocks):
        draws = jax.random.uniform(jax.random.fold_in(jax.random.fold_in(key, 6), dim), (blocks,), jnp.float32, low / len(pieces), top_value / len(pieces))
        return jnp.repeat(jnp.exp(draws), extent[dim] // blocks).reshape((-1,) + (1,) * (len(extent) - dim - 1))

    loudness = one(*pieces[0])
    for cut in pieces[1:]:
        loudness = loudness * one(*cut)
    return loudness


def normal_values(stream_key, extent, spread, most, split=(), kind=jnp.bfloat16):
    result = jax.random.normal(stream_key, extent, jnp.float32) * spread
    if len(split) > 0:
        result = block_levels(stream_key, extent, split, -0.22, 0.18) * result
    return jnp.clip(result, min=-most, max=most).astype(kind)


def gaussian_with(own_key, shape, deviation, reach, pieces, heavy, kind=jnp.bfloat16):
    drawn = deviation * jax.random.normal(own_key, shape, jnp.float32)
    if pieces:
        drawn = drawn * block_levels(own_key, shape, pieces, -0.22, 0.18)
    return jnp.clip(strengthened(drawn, jax.random.fold_in(own_key, 3), *heavy), -reach, reach).astype(kind)


def setup_inputs(seed: int = 0) -> dict:
    key_of = jax.random.split(jax.random.key(seed), 5)
    inputs = gaussian_with(key_of[0], (TOKENS, D), 1.0, 6.0, ((0, 16),), (0, 1, 16, 2.0))
    w_up = normal_values(key_of[1], (D, FF), D ** -0.5, 0.125, ((0, 8), (1, 2)))
    w_down = normal_values(key_of[2], (FF, D), FF ** -0.5, 0.09375, ((0, 2), (1, 8)))
    cotangent = gaussian_with(key_of[3], (TOKENS, D), 1.0, 6.0, ((0, 16),), (0, 1, 16, 2.0))
    return {"inputs": inputs, "w_up": w_up, "w_down": w_down, "cotangent": cotangent}


def reference(inputs, w_up, w_down, cotangent):
    preact = jnp.dot(inputs, w_up, preferred_element_type=jnp.float32)
    grad_hidden = jnp.dot(cotangent, w_down.T, preferred_element_type=jnp.float32)
    grad_pre = (2.0 * jnp.maximum(preact, 0.0) * grad_hidden).astype(jnp.bfloat16)
    tp_cols = FF // N_TP
    accumulated = jnp.zeros(inputs.shape, jnp.float32)
    for shard_index in range(N_TP):
        lower = shard_index * tp_cols
        partial_sum = jnp.dot(grad_pre[:, lower:lower + tp_cols], w_up[:, lower:lower + tp_cols].T,
                              preferred_element_type=jnp.float32).astype(jnp.bfloat16)
        accumulated = accumulated + partial_sum.astype(jnp.float32)
    d_inputs = accumulated.astype(jnp.bfloat16)
    d_w_up = jnp.dot(inputs.T, grad_pre, preferred_element_type=jnp.float32)
    return d_inputs, d_w_up
```

```python
import jax
import jax.numpy as jnp
from jax import lax
from jax.sharding import PartitionSpec as P


def per_device(inputs, w_up, w_down, cotangent):
    n_rep = lax.axis_size("rep")
    rep = lax.axis_index("rep")
    tokens = inputs.shape[0]
    hidden = w_up.shape[1] // n_rep

    def from_rep(value, step):
        return lax.ppermute(value, "rep", [((r + step) % n_rep, r) for r in range(n_rep)])

    up_block = lax.dynamic_slice_in_dim(w_up, rep * hidden, hidden, axis=1)
    down_block = lax.dynamic_slice_in_dim(w_down, rep * hidden, hidden, axis=0)
    up_whole = lax.all_gather(up_block, "fs", axis=0, tiled=True)
    down_whole = lax.all_gather(down_block, "fs", axis=1, tiled=True)
    rows = jnp.concatenate([inputs] + [from_rep(inputs, k) for k in range(1, n_rep)], axis=0)
    cots = jnp.concatenate([cotangent] + [from_rep(cotangent, k) for k in range(1, n_rep)], axis=0)
    preact = jnp.dot(rows, up_whole, preferred_element_type=jnp.float32)
    grad_hidden = lax.dot_general(
        cots, down_whole, (((1,), (1,)), ((), ())), preferred_element_type=jnp.float32
    )
    grad_pre = (2.0 * jnp.maximum(preact, 0.0) * grad_hidden).astype(jnp.bfloat16)
    d_w = lax.dot_general(
        rows, grad_pre, (((0,), (0,)), ((), ())), preferred_element_type=jnp.float32
    ).astype(jnp.bfloat16)
    own_rows = lax.psum_scatter(d_w, "fs", scatter_dimension=0, tiled=True)
    partial_value = lax.dot_general(
        grad_pre, up_whole, (((1,), (1,)), ((), ())), preferred_element_type=jnp.float32
    )
    own = partial_value[:tokens]
    for k in range(1, n_rep):
        mine = partial_value[k * tokens:(k + 1) * tokens].astype(jnp.bfloat16)
        own = own + from_rep(mine, n_rep - k).astype(jnp.float32)
    d_inputs = lax.psum(own.astype(jnp.bfloat16), "tp")
    whole_rows = jnp.zeros((own_rows.shape[0], w_up.shape[1]), jnp.float32)
    for k in range(n_rep):
        block = own_rows if k == 0 else from_rep(own_rows, k)
        at = lax.rem(rep + k, n_rep) * hidden
        whole_rows = lax.dynamic_update_slice_in_dim(whole_rows, block.astype(jnp.float32), at, axis=1)
    return (d_inputs, whole_rows)


def solution(mesh):
    in_specs = (P(("rep", "fs"), None), P("fs", "tp"), P("tp", "fs"), P(("rep", "fs"), None))
    out_specs = (P(("rep", "fs"), None), P("fs", "tp"))
    return jax.shard_map(
        per_device, mesh=mesh, in_specs=in_specs, out_specs=out_specs, check_vma=False
    )
```

```python
import functools

import jax
import jax.numpy as jnp
from jax import lax
from jax.experimental import pallas as pl
from jax.experimental.pallas import tpu as pltpu
from jax.sharding import PartitionSpec as P

MESH = pl.DeviceIdType.MESH


def gather_kernel(line, x_ref, c_ref, w_ref, wall_ref, tx_ref, tc_ref, zs, zr, ys, yr, ts, tr, cs, cr):
    r, f, c = lax.axis_index("rep"), lax.axis_index("fs"), lax.axis_index("tp")
    p, at = lax.rem(f, 2), lax.div(f, 2)
    core = lax.rem(c, 2)
    f_other = f + 1 - 2 * p
    to_x, to_y, to_core = {"rep": 1 - r}, {"fs": f_other}, {"tp": c + 1 - 2 * core}
    up, down = {"fs": f + 2}, {"fs": f - 2}
    has_up, has_down = at < line - 1, at > 0

    barrier = pltpu.get_barrier_semaphore()
    for dev in (to_x, to_y, to_core):
        pl.semaphore_signal(barrier, inc=1, device_id=dev, device_id_type=MESH)

    @pl.when(has_up)
    def _():
        pl.semaphore_signal(barrier, inc=1, device_id=up, device_id_type=MESH)

    @pl.when(has_down)
    def _():
        pl.semaphore_signal(barrier, inc=1, device_id=down, device_id_type=MESH)

    inner = has_up & has_down

    @pl.when(inner)
    def _():
        pl.semaphore_wait(barrier, 5)

    @pl.when(jnp.logical_not(inner))
    def _():
        pl.semaphore_wait(barrier, 4 if line > 1 else 3)

    def remote(src, dst, send, recv, dev):
        return pltpu.make_async_remote_copy(
            src_ref=src, dst_ref=dst, send_sem=send, recv_sem=recv, device_id=dev, device_id_type=MESH
        )

    half = x_ref.shape[0] // 2
    mine = pl.ds(pl.multiple_of(core * half, half), half)
    theirs = pl.ds(pl.multiple_of((1 - core) * half, half), half)
    toks = (tx_ref, tc_ref)

    y_copy = remote(w_ref.at[1 - p], wall_ref.at[:, f], ys, yr, to_y)
    y_copy.start()

    def z_copy(go_up, s, j):
        owner = (at - s if go_up else at + s) * 2 + (p if j == 0 else 1 - p)
        src = w_ref.at[p] if (s == 0 and j == 0) else wall_ref.at[:, owner]
        d = 0 if go_up else 1
        return remote(src, wall_ref.at[:, owner], zs.at[d, s, j], zr.at[d, s, j], up if go_up else down)

    def valid(go_up, s):
        return ((at - s >= 0) & has_up) if go_up else ((at + s < line) & has_down)

    def arrived(go_up, s):
        return (at - s >= 0) if go_up else (at + s < line)

    def z_step(s, j):
        for go_up in (True, False):
            d = 0 if go_up else 1
            if s > 0:
                @pl.when(arrived(go_up, s))
                def _():
                    owner = (at - s if go_up else at + s) * 2 + (p if j == 0 else 1 - p)
                    blk = wall_ref.at[:, owner]
                    remote(blk, blk, zs.at[d, s - 1, j], zr.at[d, s - 1, j], to_x).wait_recv()
            if s < line - 1:
                @pl.when(valid(go_up, s))
                def _():
                    z_copy(go_up, s, j).start()

    z_step(0, 0)

    own = (x_ref, c_ref)
    x_first = [remote(own[a].at[mine], toks[a].at[0, mine], ts.at[0, a], tr.at[0, a], to_x) for a in (0, 1)]
    y_first = [remote(own[a].at[mine], toks[a].at[1, mine], ts.at[1, a], tr.at[1, a], to_y) for a in (0, 1)]
    x_first[0].start()
    y_first[1].start()
    x_first[1].start()
    y_first[0].start()
    diag = [
        remote(tx_ref.at[0, mine], tx_ref.at[2, mine], ts.at[2, 0], tr.at[2, 0], to_y),
        remote(tc_ref.at[1, mine], tc_ref.at[2, mine], ts.at[2, 1], tr.at[2, 1], to_x),
    ]

    def swap(slot, a):
        return remote(toks[a].at[slot, mine], toks[a].at[slot, mine], cs.at[slot, a], cr.at[slot, a], to_core)

    y_copy.wait_recv()
    z_step(0, 1)

    def tokens_first():
        x_first[0].wait_recv()
        diag[0].start()
        swap(0, 0).start()
        y_first[1].wait_recv()
        diag[1].start()
        swap(1, 1).start()

    def tokens_second():
        x_first[1].wait_recv()
        swap(0, 1).start()
        y_first[0].wait_recv()
        swap(1, 0).start()

    todo = [tokens_first, tokens_second]
    for s in range(1, line):
        for j in (0, 1):
            z_step(s, j)
        if todo:
            todo.pop(0)()
    for more in todo:
        more()
    for a in (0, 1):
        diag[a].wait_recv()
        swap(2, a).start()
    for slot in range(3):
        for a in (0, 1):
            blk = toks[a].at[slot, theirs]
            remote(blk, blk, cs.at[slot, a], cr.at[slot, a], to_core).wait_recv()
    for slot in range(3):
        for a in (0, 1):
            swap(slot, a).wait_send()
    for copy in x_first + y_first + diag + [y_copy]:
        copy.wait_send()
    for s in range(line - 1):
        for j in (0, 1):
            for go_up in (True, False):
                @pl.when(valid(go_up, s))
                def _():
                    z_copy(go_up, s, j).wait_send()


def gather(n_fs, x, c, w):
    line = n_fs // 2
    tokens, width = x.shape
    rows, cols = w.shape[2:]
    dma = pltpu.SemaphoreType.DMA
    hbm = pl.BlockSpec(memory_space=pl.ANY)
    return pl.pallas_call(
        functools.partial(gather_kernel, line),
        out_shape=(
            jax.ShapeDtypeStruct((2, n_fs, rows, cols), w.dtype),
            jax.ShapeDtypeStruct((3, tokens, width), x.dtype),
            jax.ShapeDtypeStruct((3, tokens, width), c.dtype),
        ),
        in_specs=[hbm] * 3,
        out_specs=(hbm,) * 3,
        scratch_shapes=[
            dma((2, line, 2)), dma((2, line, 2)), dma, dma,
            dma((3, 2)), dma((3, 2)), dma((3, 2)), dma((3, 2)),
        ],
        compiler_params=pltpu.CompilerParams(collective_id=0, has_side_effects=True),
    )(x, c, w)


def per_device(inputs, w_up, w_down, cotangent):
    n_rep, n_fs, n_tp = lax.axis_size("rep"), lax.axis_size("fs"), lax.axis_size("tp")
    rep, fs, tp = lax.axis_index("rep"), lax.axis_index("fs"), lax.axis_index("tp")
    pair = lax.rem(fs, 2)
    tokens, width = inputs.shape
    rows, block = w_up.shape
    hq = block // (n_rep * 2)
    f32, bf16 = jnp.float32, jnp.bfloat16

    both = lax.dynamic_slice_in_dim(w_up, rep * 2 * hq, 2 * hq, axis=1)
    both_down = lax.dynamic_slice_in_dim(w_down, rep * 2 * hq, 2 * hq, axis=0)
    w = jnp.stack([both.reshape(rows, 2, hq), both_down.T.reshape(rows, 2, hq)])
    w = w.transpose(2, 0, 1, 3)
    wall, tx, tc = gather(n_fs, inputs, cotangent, w)
    own_w = lax.dynamic_index_in_dim(w, pair, axis=0, keepdims=False)
    wall = lax.dynamic_update_slice(wall, own_w[:, None], (0, fs, 0, 0))
    up = wall[0].reshape(width, hq)
    down = wall[1].reshape(width, hq)
    tx, tc = tx.reshape(3 * tokens, width), tc.reshape(3 * tokens, width)

    def dot(a, b, da, db):
        return lax.dot_general(a, b, (((da,), (db,)), ((), ())), preferred_element_type=f32)

    def grad(x, c):
        return (2.0 * jnp.maximum(dot(x, up, 1, 0), 0.0) * dot(c, down, 1, 0)).astype(bf16)

    g_own, g_far = grad(inputs, cotangent), grad(tx, tc)
    d_w = (dot(inputs, g_own, 0, 0) + dot(tx, g_far, 0, 0)).astype(bf16)
    groups = [[2 * k + j for k in range(n_fs // 2)] for j in range(2)]
    two = lax.psum_scatter(d_w, "fs", scatter_dimension=0, axis_index_groups=groups, tiled=True)

    everyone = [(a, b) for a in range(n_rep) for b in range(n_fs)]

    def quad(value, dr, dp):
        moves = [(a * n_fs + b, ((a + dr) % n_rep) * n_fs + (b ^ dp)) for a, b in everyone]
        return lax.ppermute(value, ("rep", "fs"), moves)

    part = tokens // n_tp
    p_own, p_far = dot(g_own, up, 1, 1), dot(g_far, up, 1, 1)
    whole = jnp.concatenate([p_own[None], p_far.reshape(3, tokens, width)]).astype(bf16)
    whole = whole.reshape(4, n_tp, part, width)

    def tp_from(value, k):
        return lax.ppermute(value, "tp", [((i + k) % n_tp, i) for i in range(n_tp)])

    def part_of(k):
        return lax.dynamic_index_in_dim(whole, lax.rem(tp + k, n_tp), axis=1, keepdims=False)

    total = part_of(0).astype(f32)
    for k in range(1, n_tp):
        total = total + tp_from(part_of(n_tp - k), k).astype(f32)
    acc = total[0]
    for i, (dr, dp) in enumerate([(1, 0), (0, 1), (1, 1)]):
        acc = acc + quad(total[i + 1].astype(bf16), dr, dp).astype(f32)
    acc = acc.astype(bf16)
    d_inputs = jnp.zeros((tokens, width), bf16)
    for k in range(n_tp):
        piece = acc if k == 0 else tp_from(acc, k)
        d_inputs = lax.dynamic_update_slice_in_dim(d_inputs, piece, lax.rem(tp + k, n_tp) * part, axis=0)

    two = two.reshape(2, rows, hq)
    keep = lax.dynamic_index_in_dim(two, pair, axis=0, keepdims=False)
    give = lax.dynamic_index_in_dim(two, 1 - pair, axis=0, keepdims=False)
    d_w_up = jnp.zeros((rows, block), f32)
    for dr in range(n_rep):
        for dp in range(2):
            piece = give if dp else keep
            if dr or dp:
                piece = quad(piece, dr, dp)
            q = lax.rem(rep + dr, n_rep) * 2 + (1 - pair if dp else pair)
            d_w_up = lax.dynamic_update_slice_in_dim(d_w_up, piece.astype(f32), q * hq, axis=1)
    return (d_inputs, d_w_up)


def solution(mesh):
    in_specs = (P(("rep", "fs"), None), P("fs", "tp"), P("tp", "fs"), P(("rep", "fs"), None))
    out_specs = (P(("rep", "fs"), None), P("fs", "tp"))
    return jax.shard_map(
        per_device, mesh=mesh, in_specs=in_specs, out_specs=out_specs, check_vma=False
    )
```

```python
import functools

import jax
import jax.numpy as jnp
from jax import lax
from jax.experimental import pallas as pl
from jax.experimental.pallas import tpu as pltpu
from jax.sharding import PartitionSpec as P

MESH = pl.DeviceIdType.MESH


def gather_kernel(line, x_ref, c_ref, w_ref, up_ref, down_ref, tx_ref, tc_ref, zs, zr, ys, yr, ts, tr, cs, cr, ls):
    r, f, c = lax.axis_index("rep"), lax.axis_index("fs"), lax.axis_index("tp")
    p, at = lax.rem(f, 2), lax.div(f, 2)
    core = lax.rem(c, 2)
    f_other = f + 1 - 2 * p
    to_x, to_y, to_core = {"rep": 1 - r}, {"fs": f_other}, {"tp": c + 1 - 2 * core}
    up, down = {"fs": f + 2}, {"fs": f - 2}
    has_up, has_down = at < line - 1, at > 0

    barrier = pltpu.get_barrier_semaphore()
    for dev in (to_x, to_y, to_core):
        pl.semaphore_signal(barrier, inc=1, device_id=dev, device_id_type=MESH)

    @pl.when(has_up)
    def _():
        pl.semaphore_signal(barrier, inc=1, device_id=up, device_id_type=MESH)

    @pl.when(has_down)
    def _():
        pl.semaphore_signal(barrier, inc=1, device_id=down, device_id_type=MESH)

    inner = has_up & has_down

    @pl.when(inner)
    def _():
        pl.semaphore_wait(barrier, 5)

    @pl.when(jnp.logical_not(inner))
    def _():
        pl.semaphore_wait(barrier, 4 if line > 1 else 3)

    def remote(src, dst, send, recv, dev):
        return pltpu.make_async_remote_copy(
            src_ref=src, dst_ref=dst, send_sem=send, recv_sem=recv, device_id=dev, device_id_type=MESH
        )

    half = x_ref.shape[0] // 2
    mine = pl.ds(pl.multiple_of(core * half, half), half)
    theirs = pl.ds(pl.multiple_of((1 - core) * half, half), half)
    toks = (tx_ref, tc_ref)

    walls = (up_ref, down_ref)
    y_copies = [remote(w_ref.at[1 - p, u], walls[u].at[f], ys.at[u], yr.at[u], to_y) for u in (0, 1)]
    locals_ = [pltpu.make_async_copy(w_ref.at[p, u], walls[u].at[f], ls.at[u]) for u in (0, 1)]
    for copy in y_copies:
        copy.start()

    def z_copy(go_up, s, j):
        u, own_pair = j % 2, j < 2
        owner = (at - s if go_up else at + s) * 2 + (p if own_pair else 1 - p)
        src = w_ref.at[p, u] if (s == 0 and own_pair) else walls[u].at[owner]
        d = 0 if go_up else 1
        return remote(src, walls[u].at[owner], zs.at[d, s, j], zr.at[d, s, j], up if go_up else down)

    def valid(go_up, s):
        return ((at - s >= 0) & has_up) if go_up else ((at + s < line) & has_down)

    def arrived(go_up, s):
        return (at - s >= 0) if go_up else (at + s < line)

    def z_step(s, j):
        for go_up in (True, False):
            d = 0 if go_up else 1
            if s > 0:
                @pl.when(arrived(go_up, s))
                def _():
                    owner = (at - s if go_up else at + s) * 2 + (p if j < 2 else 1 - p)
                    blk = walls[j % 2].at[owner]
                    remote(blk, blk, zs.at[d, s - 1, j], zr.at[d, s - 1, j], to_x).wait_recv()
            if s < line - 1:
                @pl.when(valid(go_up, s))
                def _():
                    z_copy(go_up, s, j).start()

    z_step(0, 0)
    z_step(0, 1)

    own = (x_ref, c_ref)
    x_first = [remote(own[a].at[mine], toks[a].at[0, mine], ts.at[0, a], tr.at[0, a], to_x) for a in (0, 1)]
    y_first = [remote(own[a].at[mine], toks[a].at[1, mine], ts.at[1, a], tr.at[1, a], to_y) for a in (0, 1)]
    x_first[0].start()
    y_first[1].start()
    x_first[1].start()
    y_first[0].start()
    diag = [
        remote(tx_ref.at[0, mine], tx_ref.at[2, mine], ts.at[2, 0], tr.at[2, 0], to_y),
        remote(tc_ref.at[1, mine], tc_ref.at[2, mine], ts.at[2, 1], tr.at[2, 1], to_x),
    ]

    def swap(slot, a):
        return remote(toks[a].at[slot, mine], toks[a].at[slot, mine], cs.at[slot, a], cr.at[slot, a], to_core)

    for copy in locals_:
        copy.start()
    for u in (0, 1):
        y_copies[u].wait_recv()
        z_step(0, 2 + u)

    def tokens_first():
        x_first[0].wait_recv()
        diag[0].start()
        swap(0, 0).start()
        y_first[1].wait_recv()
        diag[1].start()
        swap(1, 1).start()

    def tokens_second():
        x_first[1].wait_recv()
        swap(0, 1).start()
        y_first[0].wait_recv()
        swap(1, 0).start()

    todo = [tokens_first, tokens_second]
    for s in range(1, line):
        for j in range(4):
            z_step(s, j)
        if todo:
            todo.pop(0)()
    for more in todo:
        more()
    for a in (0, 1):
        diag[a].wait_recv()
        swap(2, a).start()
    for slot in range(3):
        for a in (0, 1):
            blk = toks[a].at[slot, theirs]
            remote(blk, blk, cs.at[slot, a], cr.at[slot, a], to_core).wait_recv()
    for slot in range(3):
        for a in (0, 1):
            swap(slot, a).wait_send()
    for copy in x_first + y_first + diag + y_copies:
        copy.wait_send()
    for s in range(line - 1):
        for j in range(4):
            for go_up in (True, False):
                @pl.when(valid(go_up, s))
                def _():
                    z_copy(go_up, s, j).wait_send()
    for copy in locals_:
        copy.wait()


def gather(n_fs, x, c, w):
    line = n_fs // 2
    tokens, width = x.shape
    rows, cols = w.shape[2:]
    dma = pltpu.SemaphoreType.DMA
    hbm = pl.BlockSpec(memory_space=pl.ANY)
    return pl.pallas_call(
        functools.partial(gather_kernel, line),
        out_shape=(
            jax.ShapeDtypeStruct((n_fs, rows, cols), w.dtype),
            jax.ShapeDtypeStruct((n_fs, rows, cols), w.dtype),
            jax.ShapeDtypeStruct((3, tokens, width), x.dtype),
            jax.ShapeDtypeStruct((3, tokens, width), c.dtype),
        ),
        in_specs=[hbm] * 3,
        out_specs=(hbm,) * 4,
        scratch_shapes=[
            dma((2, line, 4)), dma((2, line, 4)), dma((2,)), dma((2,)),
            dma((3, 2)), dma((3, 2)), dma((3, 2)), dma((3, 2)), dma((2,)),
        ],
        compiler_params=pltpu.CompilerParams(collective_id=0, has_side_effects=True),
    )(x, c, w)


def per_device(inputs, w_up, w_down, cotangent):
    n_rep, n_fs, n_tp = lax.axis_size("rep"), lax.axis_size("fs"), lax.axis_size("tp")
    rep, fs, tp = lax.axis_index("rep"), lax.axis_index("fs"), lax.axis_index("tp")
    pair = lax.rem(fs, 2)
    tokens, width = inputs.shape
    rows, block = w_up.shape
    hq = block // (n_rep * 2)
    f32, bf16 = jnp.float32, jnp.bfloat16

    both = lax.dynamic_slice_in_dim(w_up, rep * 2 * hq, 2 * hq, axis=1)
    both_down = lax.dynamic_slice_in_dim(w_down, rep * 2 * hq, 2 * hq, axis=0)
    w = jnp.stack([both.reshape(rows, 2, hq), both_down.T.reshape(rows, 2, hq)])
    w = w.transpose(2, 0, 1, 3)
    up, down, tx, tc = gather(n_fs, inputs, cotangent, w)
    up, down = up.reshape(width, hq), down.reshape(width, hq)
    tx, tc = tx.reshape(3 * tokens, width), tc.reshape(3 * tokens, width)

    def dot(a, b, da, db):
        return lax.dot_general(a, b, (((da,), (db,)), ((), ())), preferred_element_type=f32)

    def grad(x, c):
        return (2.0 * jnp.maximum(dot(x, up, 1, 0), 0.0) * dot(c, down, 1, 0)).astype(bf16)

    g_own, g_far = grad(inputs, cotangent), grad(tx, tc)
    d_w = (dot(inputs, g_own, 0, 0) + dot(tx, g_far, 0, 0)).astype(bf16)
    line, at = n_fs // 2, lax.div(fs, 2)
    pieces = [
        lax.dynamic_slice_in_dim(d_w, lax.rem(at + k, line) * 2 * rows, 2 * rows, axis=0)
        for k in range(line)
    ]
    g_own, g_far, pieces = lax.optimization_barrier((g_own, g_far, pieces))
    two = pieces[0].astype(f32)
    for k in range(1, line):
        two = two + lax.ppermute(pieces[k], "fs", [(i, (i + 2 * k) % n_fs) for i in range(n_fs)]).astype(f32)
    two = two.astype(bf16)

    everyone = [(a, b) for a in range(n_rep) for b in range(n_fs)]

    def quad(value, dr, dp):
        moves = [(a * n_fs + b, ((a + dr) % n_rep) * n_fs + (b ^ dp)) for a, b in everyone]
        return lax.ppermute(value, ("rep", "fs"), moves)

    part = tokens // n_tp
    p_own, p_far = dot(g_own, up, 1, 1), dot(g_far, up, 1, 1)
    whole = jnp.concatenate([p_own[None], p_far.reshape(3, tokens, width)]).astype(bf16)
    whole = whole.reshape(4, n_tp, part, width)

    def tp_from(value, k):
        return lax.ppermute(value, "tp", [((i + k) % n_tp, i) for i in range(n_tp)])

    def part_of(k):
        return lax.dynamic_index_in_dim(whole, lax.rem(tp + k, n_tp), axis=1, keepdims=False)

    total = part_of(0).astype(f32)
    for k in range(1, n_tp):
        total = total + tp_from(part_of(n_tp - k), k).astype(f32)
    acc = total[0]
    for i, (dr, dp) in enumerate([(1, 0), (0, 1), (1, 1)]):
        acc = acc + quad(total[i + 1].astype(bf16), dr, dp).astype(f32)
    acc = acc.astype(bf16)
    pieces = [acc] + [tp_from(acc, k) for k in range(1, n_tp)]
    parts = []
    for i in range(n_tp):
        chosen = pieces[0]
        for k in range(1, n_tp):
            chosen = jnp.where(lax.rem(tp + k, n_tp) == i, pieces[k], chosen)
        parts.append(chosen)
    d_inputs = jnp.concatenate(parts, axis=0)

    keep = lax.dynamic_slice_in_dim(two, pair * rows, rows, axis=0)
    give = lax.dynamic_slice_in_dim(two, (1 - pair) * rows, rows, axis=0)
    far = {(dr, dp): quad(give if dp else keep, dr, dp) for dr, dp in [(1, 1), (1, 0), (0, 1)]}
    far[0, 0] = keep
    quarters = []
    for a in range(n_rep):
        for b in range(2):
            by_pair = [jnp.where(pair == b, far[dr, 0], far[dr, 1]) for dr in range(2)]
            quarters.append(jnp.where(rep == a, by_pair[0], by_pair[1]).astype(f32))
    d_w_up = jnp.concatenate(quarters, axis=1)
    return (d_inputs, d_w_up)


def solution(mesh):
    in_specs = (P(("rep", "fs"), None), P("fs", "tp"), P("tp", "fs"), P(("rep", "fs"), None))
    out_specs = (P(("rep", "fs"), None), P("fs", "tp"))
    return jax.shard_map(
        per_device, mesh=mesh, in_specs=in_specs, out_specs=out_specs, check_vma=False
    )
```
